32 devices in a mesh: ep: 8 (over z, y), tp: 4 (over x, core).
Axes of the slice: x: 2, y: 2, z: 4, core: 2. Of those that a mesh axis runs over, the one named last changes fastest.
Arguments:
- q_latent: bfloat16 [4096, 512], P(('ep', 'tp')), may hold values from -6 to 6
- kv_latent: bfloat16 [4096, 256], P(('ep', 'tp')), may hold values from -6 to 6
- rope_key: bfloat16 [4096, 32], P(('ep', 'tp')), may hold values from -240 to 240
- q_gain: float32 [512], replicated, may hold values from 0.1 to 1.9
- kv_gain: float32 [256], replicated, may hold values from 0.1 to 1.9
- w_query: bfloat16 [512, 1024], P(None, 'tp'), may hold values from -0.25 to 0.25
- w_query_rot: bfloat16 [512, 512], P(None, 'tp'), may hold values from -0.25 to 0.25
- w_key: bfloat16 [256, 1024], P(None, 'tp'), may hold values from -0.375 to 0.375
- w_value: bfloat16 [256, 1024], P(None, 'tp'), may hold values from -0.375 to 0.375
- w_mix_out: bfloat16 [1024, 2048], P('tp'), may hold values from -0.1875 to 0.1875
- expert_input: bfloat16 [4096, 2048], P(('ep', 'tp')), may hold values from -6 to 6
- ffn_gain: float32 [2048], replicated, may hold values from 0.1 to 1.9
- expert_ids: int32 [4096, 4], P(('ep', 'tp')), may hold values from 0 to 7, all different within a row; in each aligned block of 128 rows (0 to 127, 128 to 255, ...) at most 96 rows name the same one
- route_weights: float32 [4096, 4], P(('ep', 'tp')), may hold values from 0.2 to 1
- w_gate_exp: bfloat16 [8, 2048, 1024], P('ep', None, 'tp'), may hold values from -0.125 to 0.125
- w_up_exp: bfloat16 [8, 2048, 1024], P('ep', None, 'tp'), may hold values from -0.125 to 0.125
- w_down_exp: bfloat16 [8, 1024, 2048], P('ep', 'tp'), may hold values from -0.1875 to 0.1875
Outputs:
- mixer_out: bfloat16 [4096, 2048], P(('ep', 'tp'))
- expert_out: bfloat16 [4096, 2048], P(('ep', 'tp'))
The draws below stay inside these ranges and needn't reach their ends.
Inputs may be any that keep to these rules, and one draw needn't show every extreme that they name: `expert_ids`: the experts of a row are all different. In the rows of one device (aligned blocks of 128 tokens) no expert is named by more than 96 rows, a bound that some block reaches.
All inputs are finite; a program needn't handle non-finite values.
Results may differ from the reference program's by a relative error of at most 0.012.
The reference program's roundings to bfloat16 on the way count: a program that leaves them out, or rounds other values in their place, can miss the bound.
Values may be sent and summed in bfloat16 or wider, within the bound.
A program may use at most 128 MiB of HBM per device.

```python
import math
import jax
import jax.numpy as jnp
import numpy as np
from jax import lax

D = 2048
HEADS = 16
NOPE = 64
ROPE = 32
VD = 64
Q_RANK = 512
KV_RANK = 256
FF = 1024
TOPK = 4
SEG = 64
TOK_DEV = 128
EXPERTS = 8
TOKENS = 4096
CAP = 96
N_EP = 8
N_TP = 4


def draw_rope_key(key, part):
    drawn = jnp.clip(jax.random.normal(jax.random.fold_in(key, 11), (TOKENS, ROPE), jnp.float32), -6.0, 6.0)
    return drawn.astype(jnp.bfloat16)


def levels(key, dims, split, least, high):
    loudness = 1.0
    for position, blocks in split:
        steps = jax.random.uniform(jax.random.fold_in(jax.random.fold_in(key, 6), position), (blocks,), jnp.float32, least / len(split), high / len(split))
        loudness = loudness * jnp.repeat(jnp.exp(steps), dims[position] // blocks).reshape((-1,) + (1,) * (len(dims) - 1 - position))
    return loudness


def deal_out(key, own, number, rows, number_of, top, bound, skew):
    order = jax.random.permutation(key, number_of)
    packed, ordinary = shares(number_of, rows * top, bound, skew, True), shares(number_of, rows * top, bound, skew, False)
    places = jnp.arange(number_of)

    def named(tallies, offset_by):
        used = int((tallies > 0).sum())
        fixed = max(1, used // 4)
        moved = fixed + (places - fixed + offset_by * (used - fixed)) % max(1, number_of - fixed)
        return jnp.zeros((number_of,), jnp.int32).at[order[jnp.where(places < fixed, places, moved)]].set(jnp.asarray(tallies, jnp.int32))

    tallies = jnp.where(number % 4 == 0, named(packed, number // 4), named(ordinary, number - number // 4 - 1))
    mixed = jax.random.permutation(jax.random.fold_in(own, 3), number_of)
    giver, taker = mixed[0:number_of // 2 * 2:2], mixed[1:number_of // 2 * 2:2]
    slack = jnp.minimum(tallies[giver] - 1, bound - tallies[taker]) // 2
    slack = jnp.where((giver == order[0]) | (taker == order[0]) | (tallies[taker] == 0), 0, jnp.maximum(slack, 0))
    moved = jax.random.randint(jax.random.fold_in(own, 4), (number_of // 2,), 0, 1 << 20) % (slack + 1)
    tallies = tallies.at[giver].add(-moved).at[taker].add(moved)
    members = jnp.searchsorted(jnp.cumsum(tallies), jnp.arange(rows * top), side="right").astype(jnp.int32)
    grid = members.reshape(top, rows).T
    grid = grid[jax.random.permutation(jax.random.fold_in(own, 1), rows)]
    offset_by = jax.random.randint(jax.random.fold_in(own, 2), (rows, 1), 0, top)
    return jnp.take_along_axis(grid, (jnp.arange(top)[None, :] + offset_by) % top, axis=1)


def shares(amount, total, limit, lean, full):
    weights = [(1 << 20) // math.isqrt(rank ** lean) + 1 for rank in range(1, amount + 1)]
    largest = limit if full else min(limit, max(-(-total // amount), total * weights[0] // sum(weights)))
    least = 1 if total - largest >= amount - 1 else 0
    holding, surplus = [largest] + [least] * (amount - 1), total - largest - least * (amount - 1)
    while surplus > 0:
        free = [i for i in range(1, amount) if holding[i] < largest] or [i for i in range(1, amount) if holding[i] < limit]
        whole, budget = sum([weights[i] for i in free]), surplus
        for i in free:
            more = min(limit - holding[i], max(1, budget * weights[i] // whole), surplus)
            holding[i] = holding[i] + more
            surplus = surplus - more
    return np.array(holding)


def noise(key, dims, width, limit, split=(), kind=jnp.bfloat16):
    result = width * jax.random.normal(key, dims, jnp.float32)
    if split:
        result = result * levels(key, dims, split, -0.22, 0.18)
    return jnp.clip(result, -limit, limit).astype(kind)


def setup_inputs(seed: int = 0) -> dict:
    keys = jax.random.split(jax.random.key(seed), 18)
    q_latent = noise(keys[0], (TOKENS, Q_RANK), 1.0, 6.0, ((0, 32),))
    kv_latent = noise(keys[1], (TOKENS, KV_RANK), 1.0, 6.0, ((0, 32),))
    rope_key = draw_rope_key(jax.random.fold_in(keys[17], 71), 0)
    q_gain = jnp.clip(1.0 + 0.18 * jax.random.normal(keys[3], (Q_RANK,), jnp.float32), 0.1, 1.9)
    kv_gain = jnp.clip(1.0 + 0.18 * jax.random.normal(keys[4], (KV_RANK,), jnp.float32), 0.1, 1.9)
    w_query = noise(keys[5], (Q_RANK, HEADS * NOPE), Q_RANK ** -0.5, 0.25, ((1, 4),))
    w_query_rot = noise(keys[6], (Q_RANK, HEADS * ROPE), Q_RANK ** -0.5, 0.25, ((1, 4),))
    w_key = noise(keys[7], (KV_RANK, HEADS * NOPE), KV_RANK ** -0.5, 0.375, ((1, 4),))
    w_value = noise(keys[8], (KV_RANK, HEADS * VD), KV_RANK ** -0.5, 0.375, ((1, 4),))
    w_mix_out = noise(keys[9], (HEADS * VD, D), (HEADS * VD) ** -0.5, 0.1875, ((0, 4),))
    expert_input = noise(keys[10], (TOKENS, D), 1.0, 6.0, ((0, 32),))
    ffn_gain = jnp.clip(1.0 + 0.18 * jax.random.normal(keys[11], (D,), jnp.float32), 0.1, 1.9)
    expert_ids_keys = jax.random.split(jax.random.fold_in(keys[12], 1), TOKENS // TOK_DEV)
    expert_ids_turns = jax.random.permutation(jax.random.fold_in(keys[12], 3), TOKENS // TOK_DEV)
    expert_ids = jax.vmap(lambda own, number: deal_out(jax.random.fold_in(keys[12], 2), own, number, TOK_DEV, EXPERTS, TOPK, CAP, 2))(expert_ids_keys, expert_ids_turns).reshape((TOKENS, TOPK))
    route_weights = jnp.clip(0.2 + 0.8 * jax.random.uniform(keys[13], (TOKENS, TOPK), jnp.float32) ** levels(keys[13], (TOKENS, TOPK), ((0, 32),), -0.2, 0.2), 0.2, 1.0)
    w_gate_exp = noise(keys[14], (EXPERTS, D, FF), D ** -0.5, 0.125, ((0, 8), (2, 4)))
    w_up_exp = noise(keys[15], (EXPERTS, D, FF), D ** -0.5, 0.125, ((0, 8), (2, 4)))
    w_down_exp = noise(keys[16], (EXPERTS, FF, D), FF ** -0.5, 0.1875, ((0, 8), (1, 4)))
    return dict(q_latent=q_latent, kv_latent=kv_latent, rope_key=rope_key, q_gain=q_gain, kv_gain=kv_gain, w_query=w_query, w_query_rot=w_query_rot, w_key=w_key, w_value=w_value, w_mix_out=w_mix_out, expert_input=expert_input, ffn_gain=ffn_gain, expert_ids=expert_ids, route_weights=route_weights, w_gate_exp=w_gate_exp, w_up_exp=w_up_exp, w_down_exp=w_down_exp)


norm_epsilon = 1e-06
rope_base = 10000.0
query_block = 256

def rms_scale(values_in, gain_vec):
    floats = values_in.astype(jnp.float32)
    return floats * lax.rsqrt(lax.optimization_barrier(jnp.mean(floats * floats, axis=-1, keepdims=True)) + norm_epsilon) * gain_vec

def tables(positions):
    half_width = ROPE // 2
    frequency = rope_base ** (-jnp.arange(half_width, dtype=jnp.float32) / half_width)
    angles = positions.astype(jnp.float32)[:, None] * frequency[None, :]
    return (jnp.cos(angles), jnp.sin(angles))

def rotate_pairs(values_in, cosine, sine_table):
    half_width = values_in.shape[-1] // 2
    first, second = (values_in[..., :half_width], values_in[..., half_width:])
    return jnp.concatenate([first * cosine - second * sine_table, first * sine_table + second * cosine], axis=-1)

def mixer(q_latent, kv_latent, rope_key, q_gain, kv_gain, w_query, w_query_rot, w_key, w_value, w_mix_out):
    row_total = q_latent.shape[0]
    positions = jnp.arange(row_total, dtype=jnp.int32)
    cosine, sine_table = tables(positions)
    q_normed = rms_scale(q_latent, q_gain).astype(jnp.bfloat16)
    q_plain = jnp.dot(q_normed, w_query, preferred_element_type=jnp.float32).astype(jnp.bfloat16)
    q_plain = q_plain.reshape(row_total, HEADS, NOPE)
    q_turned = jnp.dot(q_normed, w_query_rot, preferred_element_type=jnp.float32).reshape(row_total, HEADS, ROPE)
    q_turned = rotate_pairs(q_turned, cosine[:, None, :], sine_table[:, None, :]).astype(jnp.bfloat16)
    kv_normed = rms_scale(kv_latent, kv_gain).astype(jnp.bfloat16)
    k_plain = jnp.dot(kv_normed, w_key, preferred_element_type=jnp.float32).astype(jnp.bfloat16)
    k_plain = k_plain.reshape(row_total, HEADS, NOPE).astype(jnp.float32)
    values = jnp.dot(kv_normed, w_value, preferred_element_type=jnp.float32).astype(jnp.bfloat16)
    values = values.reshape(row_total, HEADS, VD).astype(jnp.float32)
    k_turned = rotate_pairs(rope_key.astype(jnp.float32), cosine, sine_table).astype(jnp.bfloat16).astype(jnp.float32)
    segment = positions // SEG
    score_scale = (NOPE + ROPE) ** (-0.5)

    def attend(first_row):
        block_plain = lax.dynamic_slice_in_dim(q_plain, first_row, query_block, 0).astype(jnp.float32)
        block_turned = lax.dynamic_slice_in_dim(q_turned, first_row, query_block, 0).astype(jnp.float32)
        scores = jnp.einsum('qhd,khd->hqk', block_plain, k_plain) + jnp.einsum('qhd,kd->hqk', block_turned, k_turned)
        scores = scores * score_scale
        query_segment = (first_row + jnp.arange(query_block, dtype=jnp.int32)) // SEG
        allowed = segment[None, :] <= query_segment[:, None]
        scores = jnp.where(allowed[None], scores, -jnp.inf)
        row_max = lax.optimization_barrier(jnp.max(scores, axis=-1, keepdims=True))
        weights = jnp.where(allowed[None], jnp.exp(scores - row_max), 0.0)
        weight_sum = lax.optimization_barrier(jnp.sum(weights, axis=-1))
        rounded = weights.astype(jnp.bfloat16).astype(jnp.float32)
        mixed = jnp.einsum('hqk,khd->qhd', rounded, values) / jnp.transpose(weight_sum)[:, :, None]
        return mixed.astype(jnp.bfloat16).reshape(query_block, HEADS * VD)
    starts = jnp.arange(0, row_total, query_block, dtype=jnp.int32)
    attention = lax.map(attend, starts).reshape(row_total, HEADS * VD)
    block_width = HEADS * VD // N_TP
    summed = jnp.zeros((row_total, D), jnp.float32)
    for block_index in range(N_TP):
        columns = attention[:, block_index * block_width:(block_index + 1) * block_width]
        weight_rows = w_mix_out[block_index * block_width:(block_index + 1) * block_width]
        partial_out = jnp.dot(columns, weight_rows, preferred_element_type=jnp.float32).astype(jnp.bfloat16)
        summed = summed + lax.optimization_barrier(partial_out).astype(jnp.float32)
    return summed.astype(jnp.bfloat16)

def experts(expert_input, ffn_gain, expert_ids, route_weights, w_gate_exp, w_up_exp, w_down_exp):
    row_total = expert_input.shape[0]
    groups = N_EP * N_TP
    expert_count = w_gate_exp.shape[0]
    normed = rms_scale(expert_input, ffn_gain).astype(jnp.bfloat16)
    routed = expert_ids.reshape(groups, TOK_DEV * TOPK).astype(jnp.int32)
    onehot = (routed[:, :, None] == jnp.arange(expert_count, dtype=jnp.int32)[None, None, :]).astype(jnp.int32)
    slot_number = lax.optimization_barrier(jnp.sum((jnp.cumsum(onehot, axis=1) - 1) * onehot, axis=-1)).astype(jnp.int32)
    group_index = jnp.arange(groups, dtype=jnp.int32)[:, None]
    slot_place = ((routed * groups + group_index) * CAP + slot_number).reshape(-1).astype(jnp.int32)
    token_index = group_index * TOK_DEV + jnp.arange(TOK_DEV * TOPK, dtype=jnp.int32)[None, :] // TOPK
    token_table = jnp.zeros((expert_count * groups * CAP,), jnp.int32).at[slot_place].set(token_index.reshape(-1).astype(jnp.int32))
    token_table = token_table.reshape(expert_count, groups * CAP)
    block_width = FF // N_TP

    def expert_block(arguments):
        rows_idx, gate_weight, up_weight, down_weight = arguments
        chosen = normed[rows_idx]
        gate_part = jnp.dot(chosen, gate_weight, preferred_element_type=jnp.float32)
        up_part = jnp.dot(chosen, up_weight, preferred_element_type=jnp.float32)
        hidden = (jax.nn.silu(gate_part) * up_part).astype(jnp.bfloat16)
        summed = jnp.zeros((chosen.shape[0], D), jnp.float32)
        for block_index in range(N_TP):
            columns = hidden[:, block_index * block_width:(block_index + 1) * block_width]
            weight_rows = down_weight[block_index * block_width:(block_index + 1) * block_width]
            partial_out = jnp.dot(columns, weight_rows, preferred_element_type=jnp.float32).astype(jnp.bfloat16)
            summed = summed + lax.optimization_barrier(partial_out).astype(jnp.float32)
        return summed.astype(jnp.bfloat16)
    results = lax.map(expert_block, (token_table, w_gate_exp, w_up_exp, w_down_exp))
    all_results = results.reshape(-1, D)
    picked = all_results[slot_place].astype(jnp.float32).reshape(row_total, TOPK, D)
    weighted_sum = lax.optimization_barrier(jnp.sum(picked * route_weights[:, :, None].astype(jnp.float32), axis=1))
    return weighted_sum.astype(jnp.bfloat16)

def reference(q_latent, kv_latent, rope_key, q_gain, kv_gain, w_query, w_query_rot, w_key, w_value, w_mix_out, expert_input, ffn_gain, expert_ids, route_weights, w_gate_exp, w_up_exp, w_down_exp):
    mixer_out = mixer(q_latent, kv_latent, rope_key, q_gain, kv_gain, w_query, w_query_rot, w_key, w_value, w_mix_out)
    expert_out = experts(expert_input, ffn_gain, expert_ids, route_weights, w_gate_exp, w_up_exp, w_down_exp)
    return (mixer_out, expert_out)
```

```python
import functools
import math

import jax
import jax.numpy as jnp
from jax import lax
from jax.experimental import pallas as pl
from jax.experimental.pallas import tpu as pltpu
from jax.sharding import PartitionSpec as P

D = 2048
NOPE = 64
ROPE = 32
VD = 64
TOPK = 4
SEG = 64


norm_epsilon = 1e-06
rope_base = 10000.0
masked_score = -1e30


def rms_scale(values_in, gain_vec):
    floats = values_in.astype(jnp.float32)
    return (
        floats
        * lax.rsqrt(jnp.mean(floats * floats, axis=-1, keepdims=True) + norm_epsilon)
        * gain_vec
    )


def tables(positions):
    half_width = ROPE // 2
    frequency = rope_base ** (-jnp.arange(half_width, dtype=jnp.float32) / half_width)
    angles = positions.astype(jnp.float32)[:, None] * frequency[None, :]
    return (jnp.cos(angles), jnp.sin(angles))


def rotate_pairs(values_in, cosine, sine_table):
    half_width = values_in.shape[-1] // 2
    first, second = (values_in[..., :half_width], values_in[..., half_width:])
    return jnp.concatenate(
        [first * cosine - second * sine_table, first * sine_table + second * cosine], axis=-1
    )


LANES = 128


def pad_heads(weight, heads, width):
    split = weight.reshape(weight.shape[0], heads, width)
    return jnp.pad(split, ((0, 0), (0, 0), (0, LANES - width))).reshape(
        weight.shape[0], heads * LANES
    )


def make_queries(q_rows, q_gain, w_query, w_query_rot, heads, group_rows):
    start = lax.axis_index("ep") * group_rows
    cosine, sine_table = tables(start + jnp.arange(group_rows, dtype=jnp.int32))
    normed = rms_scale(q_rows, q_gain).astype(jnp.bfloat16)
    plain = jnp.dot(normed, w_query, preferred_element_type=jnp.float32).astype(jnp.bfloat16)
    turned = jnp.dot(normed, w_query_rot, preferred_element_type=jnp.float32).reshape(
        group_rows, heads, ROPE
    )
    turned = rotate_pairs(turned, cosine[:, None, :], sine_table[:, None, :]).astype(jnp.bfloat16)
    blank = jnp.zeros((group_rows, heads, LANES - NOPE - ROPE), jnp.bfloat16)
    joined = jnp.concatenate([plain.reshape(group_rows, heads, NOPE), turned, blank], axis=-1)
    return joined.reshape(group_rows, heads * LANES)


def make_keys(kv_rows, kv_gain, w_key, w_value, heads):
    row_count = kv_rows.shape[0]
    rank = w_key.shape[0]
    normed = rms_scale(kv_rows[:, :rank], kv_gain).astype(jnp.bfloat16)
    cosine, sine_table = tables(jnp.arange(row_count, dtype=jnp.int32))
    turned = rotate_pairs(kv_rows[:, rank:].astype(jnp.float32), cosine, sine_table)
    turned = jnp.pad(
        turned.astype(jnp.bfloat16), ((0, 0), (NOPE, LANES - NOPE - ROPE))
    )
    plain = jnp.dot(normed, pad_heads(w_key, heads, NOPE), preferred_element_type=jnp.float32)
    keys = plain.astype(jnp.bfloat16) + jnp.tile(turned, (1, heads))
    raw = jnp.dot(normed, pad_heads(w_value, heads, VD), preferred_element_type=jnp.float32)
    ones = (jnp.arange(heads * LANES, dtype=jnp.int32) % LANES == VD).astype(jnp.bfloat16)
    return keys, raw.astype(jnp.bfloat16) + ones[None, :]


def attention_kernel(heads, chunk, group_ref, q_ref, k_ref, v_ref, o_ref, max_ref, acc_ref):
    step = pl.program_id(0)
    group = group_ref[0]
    rows = q_ref.shape[0]
    keys = k_ref.shape[0]
    log_scale = (NOPE + ROPE) ** (-0.5) * math.log2(math.e)

    @pl.when(step == 0)
    def _():
        max_ref[...] = jnp.full(max_ref.shape, masked_score, jnp.float32)
        acc_ref[...] = jnp.zeros(acc_ref.shape, jnp.float32)

    def work(masked):
        for head in range(heads):
            lanes = slice(head * LANES, (head + 1) * LANES)
            for first in range(0, rows, chunk):
                part = slice(first, first + chunk)
                scores = lax.dot_general(
                    q_ref[part, lanes],
                    k_ref[:, lanes],
                    (((1,), (1,)), ((), ())),
                    preferred_element_type=jnp.float32,
                )
                if masked:
                    row_id = lax.broadcasted_iota(jnp.int32, (chunk, keys), 0) + first
                    col_id = lax.broadcasted_iota(jnp.int32, (chunk, keys), 1)
                    scores = jnp.where(col_id // SEG <= row_id // SEG, scores, masked_score)
                old = max_ref[head, part, :]
                new = jnp.maximum(old, jnp.max(scores, axis=-1, keepdims=True))
                weights = jnp.exp2((scores - new[:, :1]) * log_scale).astype(jnp.bfloat16)
                factor = jnp.exp2((old - new) * log_scale)
                max_ref[head, part, :] = new
                acc_ref[head, part, :] = acc_ref[head, part, :] * factor + jnp.dot(
                    weights, v_ref[:, lanes], preferred_element_type=jnp.float32
                )

    @pl.when(step < group)
    def _():
        work(False)

    @pl.when(step == group)
    def _():
        work(True)

    @pl.when(step == pl.num_programs(0) - 1)
    def _():
        for head in range(heads):
            acc = acc_ref[head]
            o_ref[:, head * VD : (head + 1) * VD] = (
                acc[:, :VD] / acc[:, VD : VD + 1]
            ).astype(jnp.bfloat16)


def attend(queries, keys, values, heads, group_rows):
    group = lax.axis_index("ep").astype(jnp.int32).reshape(1)
    blocks = keys.shape[0] // group_rows
    width = heads * LANES
    chunk = 256 if group_rows % 256 == 0 else group_rows
    return pl.pallas_call(
        functools.partial(attention_kernel, heads, chunk),
        out_shape=jax.ShapeDtypeStruct((group_rows, heads * VD), jnp.bfloat16),
        grid_spec=pltpu.PrefetchScalarGridSpec(
            num_scalar_prefetch=1,
            grid=(blocks,),
            in_specs=[
                pl.BlockSpec((group_rows, width), lambda i, g: (0, 0)),
                pl.BlockSpec((group_rows, width), lambda i, g: (jnp.minimum(i, g[0]), 0)),
                pl.BlockSpec((group_rows, width), lambda i, g: (jnp.minimum(i, g[0]), 0)),
            ],
            out_specs=pl.BlockSpec((group_rows, heads * VD), lambda i, g: (0, 0)),
            scratch_shapes=[
                pltpu.VMEM((heads, group_rows, LANES), jnp.float32),
                pltpu.VMEM((heads, group_rows, LANES), jnp.float32),
            ],
        ),
        compiler_params=pltpu.CompilerParams(
            dimension_semantics=("arbitrary",), vmem_limit_bytes=24 * 1024 * 1024
        ),
        cost_estimate=pl.CostEstimate(
            flops=4 * heads * group_rows * keys.shape[0] * LANES * 2,
            bytes_accessed=4 * keys.shape[0] * width,
            transcendentals=heads * group_rows * keys.shape[0],
        ),
        name="attend",
    )(group, queries, keys, values)


def on_device(
    q_latent,
    kv_latent,
    rope_key,
    q_gain,
    kv_gain,
    w_query,
    w_query_rot,
    w_key,
    w_value,
    w_mix_out,
    expert_input,
    ffn_gain,
    expert_ids,
    route_weights,
    w_gate_exp,
    w_up_exp,
    w_down_exp,
):
    tok_rows = q_latent.shape[0]
    tp_count = lax.axis_size("tp")
    expert_count = lax.axis_size("ep")
    slot_count = 3 * tok_rows * TOPK // (2 * expert_count)
    group_rows = tp_count * tok_rows
    heads_here = w_key.shape[1] // NOPE

    gate_all = lax.all_gather(w_gate_exp[0], "tp", axis=0)
    up_all = lax.all_gather(w_up_exp[0], "tp", axis=0)
    down_all = lax.all_gather(w_down_exp[0], "tp", axis=0)

    normed = rms_scale(expert_input, ffn_gain).astype(jnp.bfloat16)
    routed = expert_ids.reshape(-1)
    onehot = (routed[:, None] == jnp.arange(expert_count, dtype=jnp.int32)[None, :]).astype(
        jnp.int32
    )
    slot_number = jnp.sum((jnp.cumsum(onehot, axis=0) - 1) * onehot, axis=-1)
    slot_place = (routed * slot_count + slot_number).reshape(tok_rows, TOPK)
    slot_line = jnp.arange(expert_count * slot_count, dtype=jnp.int32)
    picks = [
        (slot_place[:, route_rank][:, None] == slot_line[None, :]).astype(jnp.bfloat16)
        for route_rank in range(TOPK)
    ]
    dispatch = picks[0]
    for route_rank in range(1, TOPK):
        dispatch = dispatch + picks[route_rank]
    outgoing = lax.dot_general(
        dispatch, normed, (((0,), (0,)), ((), ())), preferred_element_type=jnp.float32
    ).astype(jnp.bfloat16)
    arrived = lax.all_to_all(
        outgoing.reshape(expert_count, slot_count, D), "ep", split_axis=0, concat_axis=0, tiled=True
    )
    rows = arrived.reshape(expert_count * slot_count, D)

    own_rows = jnp.concatenate([kv_latent, rope_key], axis=1)
    ep_rows = lax.all_gather(own_rows, "ep", axis=0, tiled=True)
    column_count = own_rows.shape[1]
    piece_width = column_count // 3 if column_count % 3 == 0 else column_count
    pieces = [
        lax.all_gather(ep_rows[:, first : first + piece_width], "tp", axis=0)
        for first in range(0, column_count, piece_width)
    ]
    kv_rows = (
        jnp.concatenate(pieces, axis=2)
        .reshape(tp_count, expert_count, tok_rows, column_count)
        .transpose(1, 0, 2, 3)
        .reshape(expert_count * group_rows, column_count)
    )
    q_rows = lax.all_gather(q_latent, "tp", axis=0, tiled=True)
    queries = make_queries(q_rows, q_gain, w_query, w_query_rot, heads_here, group_rows)
    keys, values = make_keys(kv_rows, kv_gain, w_key, w_value, heads_here)
    attention = attend(queries, keys, values, heads_here, group_rows)

    total = jnp.zeros((rows.shape[0], D), jnp.float32)
    for block in range(tp_count):
        gate_part = jnp.dot(rows, gate_all[block], preferred_element_type=jnp.float32)
        up_part = jnp.dot(rows, up_all[block], preferred_element_type=jnp.float32)
        hidden = (jax.nn.silu(gate_part) * up_part).astype(jnp.bfloat16)
        part = jnp.dot(hidden, down_all[block], preferred_element_type=jnp.float32)
        total = total + part.astype(jnp.bfloat16).astype(jnp.float32)
    summed = total.astype(jnp.bfloat16)
    results = lax.all_to_all(
        summed.reshape(expert_count, slot_count, D), "ep", split_axis=0, concat_axis=0, tiled=True
    ).reshape(expert_count * slot_count, D)

    partial_out = jnp.dot(attention, w_mix_out, preferred_element_type=jnp.float32).astype(
        jnp.bfloat16
    )
    mixer_out = lax.psum_scatter(partial_out, "tp", scatter_dimension=0, tiled=True)

    fetched = jnp.dot(
        jnp.concatenate(picks, axis=0), results, preferred_element_type=jnp.float32
    ).astype(jnp.bfloat16)
    combined = jnp.zeros((tok_rows, D), jnp.float32)
    for route_rank in range(TOPK):
        piece = fetched[route_rank * tok_rows : (route_rank + 1) * tok_rows].astype(jnp.float32)
        combined = combined + route_weights[:, route_rank : route_rank + 1] * piece
    return (mixer_out, combined.astype(jnp.bfloat16))


def solution(mesh):
    return jax.shard_map(
        on_device,
        mesh=mesh,
        in_specs=(
            P(("ep", "tp"), None),
            P(("ep", "tp"), None),
            P(("ep", "tp"), None),
            P(),
            P(),
            P(None, "tp"),
            P(None, "tp"),
            P(None, "tp"),
            P(None, "tp"),
            P("tp", None),
            P(("ep", "tp"), None),
            P(),
            P(("ep", "tp"), None),
            P(("ep", "tp"), None),
            P("ep", None, "tp"),
            P("ep", None, "tp"),
            P("ep", "tp", None),
        ),
        out_specs=(P(("ep", "tp"), None), P(("ep", "tp"), None)),
        check_vma=False,
    )
```
